32 devices in a mesh: fs: 8 (over z, y), tp: 4 (over x, core).
Axes of the slice: x: 2, y: 2, z: 4, core: 2. Of those that a mesh axis runs over, the one named last changes fastest.
Arguments:
- late_input: bfloat16 [2048, 2048], P(('fs', 'tp')), may hold values from -6 to 6
- early_input: bfloat16 [2048, 2048], P(('fs', 'tp')), may hold values from -6 to 6
- early_grad: bfloat16 [2048, 2048], P(('fs', 'tp')), may hold values from -6 to 6
- pre_gain: float32 [2048], replicated, may hold values from 0.1 to 1.9
- post_gain: float32 [2048], replicated, may hold values from 0.1 to 1.9
- gate_weight: bfloat16 [2048, 4096], P('fs', 'tp'), may hold values from -0.125 to 0.125
- up_weight: bfloat16 [2048, 4096], P('fs', 'tp'), may hold values from -0.125 to 0.125
- down_weight: bfloat16 [2048, 4096], P('fs', 'tp'), may hold values from -0.09375 to 0.09375
- gate_sum: float32 [2048, 4096], P('fs', 'tp'), may hold values from -1.8 to 1.8
- up_sum: float32 [2048, 4096], P('fs', 'tp'), may hold values from -1.8 to 1.8
- down_gradient_sum: float32 [2048, 4096], P('fs', 'tp'), may hold values from -1.8 to 1.8
Outputs:
- late_output: bfloat16 [2048, 2048], P(('fs', 'tp'))
- early_input_grad: bfloat16 [2048, 2048], P(('fs', 'tp'))
- gate_total: float32 [2048, 4096], P('fs', 'tp')
- up_total: float32 [2048, 4096], P('fs', 'tp')
- down_total: float32 [2048, 4096], P('fs', 'tp')
The draws below stay inside these ranges and needn't reach their ends.
All inputs are finite; a program needn't handle non-finite values.
Results may differ from the reference program's by a relative error of at most 0.013.
Values may be sent and summed in bfloat16 or wider, within the bound.
A program may use at most 128 MiB of HBM per device.

```python
import math
import jax
import jax.numpy as jnp
from jax import lax

D = 2048
FF = 4096
ROWS = 2048
N_TP = 4


def with_spikes(array, rng, source, target, shards_of, factor):
    def block_of(position):
        return (jnp.arange(array.shape[position]) // (array.shape[position] // shards_of)).reshape((-1,) + (1,) * (array.ndim - 1 - position))

    one_side = jax.random.permutation(rng, shards_of)[block_of(target)]
    other_side = (block_of(target) + shards_of // 2) % shards_of
    return jnp.where((block_of(source) == one_side) | (block_of(source) == other_side), factor * array, array)


def shard_levels(own_key, shape, pieces, least, top_value):
    gain, own = 1.0, jax.random.fold_in(own_key, 6)
    for dim, shards_of in pieces:
        draws = jnp.exp(jax.random.uniform(jax.random.fold_in(own, dim), (shards_of,), jnp.float32, least / len(pieces), top_value / len(pieces)))
        gain = gain * jnp.repeat(draws, shape[dim] // shards_of).reshape([-1 if axis == dim else 1 for axis in range(len(shape))])
    return gain


def gaussian(rng, shape, scale, bound, split=(), held_as=jnp.bfloat16):
    loudness = shard_levels(rng, shape, split, -0.22, 0.18) if split else 1.0
    entries = jax.random.normal(rng, shape, jnp.float32) * scale * loudness
    return jnp.minimum(jnp.maximum(entries, -bound), bound).astype(held_as)


def noise_with(stream_key, shape, spread, limit, pieces, heavy, held_as=jnp.bfloat16):
    result = spread * jax.random.normal(stream_key, shape, jnp.float32)
    if pieces:
        result = result * shard_levels(stream_key, shape, pieces, -0.22, 0.18)
    return jnp.clip(with_spikes(result, jax.random.fold_in(stream_key, 3), *heavy), -limit, limit).astype(held_as)


def setup_inputs(seed: int = 0) -> dict:
    seeds = jax.random.split(jax.random.key(seed), 12)
    late_input = gaussian(seeds[0], (ROWS, D), 1.0, 6.0, ((0, 32),))
    early_input = gaussian(seeds[1], (ROWS, D), 1.0, 6.0, ((0, 32),))
    early_grad = noise_with(seeds[2], (ROWS, D), 1.0, 6.0, ((0, 32),), (0, 1, 32, 2.75))
    pre_gain = jnp.clip(1.0 + 0.18 * jax.random.normal(seeds[3], (D,), jnp.float32), 0.1, 1.9)
    post_gain = jnp.clip(1.0 + 0.18 * jax.random.normal(seeds[4], (D,), jnp.float32), 0.1, 1.9)
    gate_weight = gaussian(seeds[5], (D, FF), D ** -0.5, 0.125, ((0, 8), (1, 4)))
    up_weight = gaussian(seeds[6], (D, FF), D ** -0.5, 0.125, ((0, 8), (1, 4)))
    down_weight = gaussian(seeds[7], (D, FF), FF ** -0.5, 0.09375, ((0, 8), (1, 4)))
    gate_sum = gaussian(seeds[8], (D, FF), 0.3, 1.8, ((0, 8), (1, 4)), jnp.float32)
    up_sum = gaussian(seeds[9], (D, FF), 0.3, 1.8, ((0, 8), (1, 4)), jnp.float32)
    down_gradient_sum = gaussian(seeds[10], (D, FF), 0.3, 1.8, ((0, 8), (1, 4)), jnp.float32)
    return dict(late_input=late_input, early_input=early_input, early_grad=early_grad, pre_gain=pre_gain, post_gain=post_gain, gate_weight=gate_weight, up_weight=up_weight, down_weight=down_weight, gate_sum=gate_sum, up_sum=up_sum, down_gradient_sum=down_gradient_sum)


NORM_EPS = 1e-06

def contract_last(first_op, second_op):
    return lax.dot_general(first_op, second_op, (((1,), (1,)), ((), ())), preferred_element_type=jnp.float32)

def contract_first(first_op, second_op):
    return lax.dot_general(first_op, second_op, (((0,), (0,)), ((), ())), preferred_element_type=jnp.float32)

def inverse_rms(values):
    return lax.rsqrt(lax.optimization_barrier(jnp.mean(values * values, axis=-1, keepdims=True)) + NORM_EPS)

def rounded_blocks(term_of, row_count):
    running = jnp.zeros((row_count, D), jnp.float32)
    for block_index in range(N_TP):
        rounded = lax.optimization_barrier(term_of(block_index).astype(jnp.bfloat16))
        running = running + rounded.astype(jnp.float32)
    return running.astype(jnp.bfloat16)

def forward_rows(input_rows, pre_gain, gate_weight, up_weight, down_weight):
    values = input_rows.astype(jnp.float32)
    normed = (values * inverse_rms(values) * pre_gain).astype(jnp.bfloat16)
    gate_pre = jnp.dot(normed, gate_weight, preferred_element_type=jnp.float32)
    up_pre = jnp.dot(normed, up_weight, preferred_element_type=jnp.float32)
    hidden_state = (jax.nn.silu(gate_pre) * up_pre).astype(jnp.bfloat16)
    block_column_count = FF // N_TP

    def term_of(block_index):
        columns = slice(block_index * block_column_count, (block_index + 1) * block_column_count)
        return contract_last(hidden_state[:, columns], down_weight[:, columns])
    mixed = rounded_blocks(term_of, input_rows.shape[0])
    return (normed, gate_pre, up_pre, hidden_state, mixed)

def reference(late_input, early_input, early_grad, pre_gain, post_gain, gate_weight, up_weight, down_weight, gate_sum, up_sum, down_gradient_sum):
    late_mixed = forward_rows(late_input, pre_gain, gate_weight, up_weight, down_weight)[4]
    late_values = late_input.astype(jnp.float32)
    mixed_values = late_mixed.astype(jnp.float32)
    late_output = (late_values + 0.5 * mixed_values * inverse_rms(mixed_values) * post_gain).astype(jnp.bfloat16)
    normed, gate_pre, up_pre, hidden_state, mixed = forward_rows(early_input, pre_gain, gate_weight, up_weight, down_weight)
    early_mixed = mixed.astype(jnp.float32)
    inverse_norm = inverse_rms(early_mixed)
    weighted = 0.5 * early_grad.astype(jnp.float32) * post_gain
    mixed_cot = (inverse_norm * weighted - early_mixed * inverse_norm ** 3 * lax.optimization_barrier(jnp.mean(weighted * early_mixed, axis=-1, keepdims=True))).astype(jnp.bfloat16)
    hidden_cot = jnp.dot(mixed_cot, down_weight, preferred_element_type=jnp.float32)
    sigmoid_gate = jax.nn.sigmoid(gate_pre)
    gate_cot = (hidden_cot * up_pre * sigmoid_gate * (1.0 + gate_pre * (1.0 - sigmoid_gate))).astype(jnp.bfloat16)
    up_cot = (hidden_cot * gate_pre * sigmoid_gate).astype(jnp.bfloat16)
    block_column_count = FF // N_TP

    def back_term(block_index):
        columns = slice(block_index * block_column_count, (block_index + 1) * block_column_count)
        return contract_last(gate_cot[:, columns], gate_weight[:, columns]) + contract_last(up_cot[:, columns], up_weight[:, columns])
    normed_cot = rounded_blocks(back_term, early_input.shape[0]).astype(jnp.float32)
    early_values = early_input.astype(jnp.float32)
    early_inverse_norm = inverse_rms(early_values)
    weighted_in = normed_cot * pre_gain
    early_input_grad = (early_grad.astype(jnp.float32) + early_inverse_norm * weighted_in - early_values * early_inverse_norm ** 3 * lax.optimization_barrier(jnp.mean(weighted_in * early_values, axis=-1, keepdims=True))).astype(jnp.bfloat16)
    grad_scale = 1.0 / math.sqrt(ROWS)
    gate_total = gate_sum + grad_scale * contract_first(normed, gate_cot)
    up_total = up_sum + grad_scale * contract_first(normed, up_cot)
    down_total = down_gradient_sum + grad_scale * contract_first(mixed_cot, hidden_state)
    return (late_output, early_input_grad, gate_total, up_total, down_total)
```

```python
import functools
import math

import jax
import jax.numpy as jnp
from jax import lax
from jax.experimental import pallas as pl
from jax.experimental.pallas import tpu as pltpu
from jax.sharding import PartitionSpec as P

NORM_EPS = 1e-06
PAIR = 2
MESH = pl.DeviceIdType.MESH
VMEM_LIMIT = 60 * 1024 * 1024


def contract_last(first_op, second_op):
    return lax.dot_general(
        first_op, second_op, (((1,), (1,)), ((), ())), preferred_element_type=jnp.float32
    )


def contract_first(first_op, second_op):
    return lax.dot_general(
        first_op, second_op, (((0,), (0,)), ((), ())), preferred_element_type=jnp.float32
    )


def inverse_rms(values):
    return lax.rsqrt(jnp.mean(values * values, axis=-1, keepdims=True) + NORM_EPS)


class Place:
    def __init__(self, n_fs, n_tp):
        self.line_len, self.n_tp = n_fs // PAIR, n_tp
        self.group = PAIR * n_tp
        self.fs, self.tp = lax.axis_index("fs"), lax.axis_index("tp")
        self.line, self.side = self.fs // PAIR, self.fs % PAIR
        self.member = self.side * n_tp + self.tp
        self.core = self.tp % PAIR
        self.chip = self.member // PAIR
        self.up = {"fs": self.fs + PAIR, "tp": self.tp}
        self.down = {"fs": self.fs - PAIR, "tp": self.tp}
        self.across = {"fs": self.line * PAIR + 1 - self.side, "tp": self.tp}
        self.has_up, self.has_down = self.line < self.line_len - 1, self.line > 0

    def member_id(self, member):
        return {"fs": self.line * PAIR + member // self.n_tp, "tp": member % self.n_tp}

    def enter(self, on_line):
        barrier = pltpu.get_barrier_semaphore()

        def greet(who):
            pl.semaphore_signal(barrier, inc=1, device_id=who, device_id_type=MESH)

        for offset in range(1, self.group):
            greet(self.member_id((self.member + offset) % self.group))
        if on_line:
            pl.when(self.has_up)(lambda: greet(self.up))
            pl.when(self.has_down)(lambda: greet(self.down))
        peers = self.group - 1
        if on_line:
            peers += self.has_up.astype(jnp.int32) + self.has_down.astype(jnp.int32)
        pl.semaphore_wait(barrier, peers)


def remote(src, dst, send_sem, recv_sem, who):
    return pltpu.make_async_remote_copy(
        src_ref=src,
        dst_ref=dst,
        send_sem=send_sem,
        recv_sem=recv_sem,
        device_id=who,
        device_id_type=MESH,
    )


def gather_kernel(
    n_fs,
    n_tp,
    late_ref,
    early_ref,
    *refs,
):
    w_refs, (late_out, early_out), w_outs = refs[:3], refs[3:5], refs[5:8]
    tok_send, tok_recv, own_sem, across_send, up_send, down_send, w_recv = refs[8:]
    at = Place(n_fs, n_tp)
    half = w_outs[0].shape[2]
    kept = pl.ds(pl.multiple_of(at.side * half, half), half)
    given = pl.ds(pl.multiple_of((1 - at.side) * half, half), half)
    at.enter(True)

    def slot_of(line, turn):
        return line * PAIR + (at.side if turn == 0 else 1 - at.side)

    def carry(w, slot, src, send_sem, who):
        return remote(src, w_outs[w].at[slot], send_sem, w_recv.at[w, slot], who)

    across, own, tokens = [], [], []
    for w in range(3):
        across.append(
            carry(w, at.fs, w_refs[w].at[:, given], across_send.at[w], at.across)
        )
        across[-1].start()
    flows = []
    for step in range(at.line_len):
        for w in range(3):
            for turn in range(PAIR):
                from_low, from_high = at.line - step, at.line + step
                low = jnp.maximum(from_low, 0)
                high = jnp.minimum(from_high, at.line_len - 1)
                flows.append((step, w, turn, from_low >= 0, from_high < at.line_len, low, high))

    def flow_copies(flow):
        step, w, turn, _, _, low, high = flow
        own_block = step == 0 and turn == 0
        copies = []
        for line, sems, who in ((low, up_send, at.up), (high, down_send, at.down)):
            slot = slot_of(line, turn)
            src = w_refs[w].at[:, kept] if own_block else w_outs[w].at[slot]
            copies.append(carry(w, slot, src, sems.at[w, step, turn], who))
        return copies

    def run(flow):
        step, w, turn, low_ok, high_ok, _, _ = flow
        up_copy, down_copy = flow_copies(flow)
        if step == 0 and turn == 1:
            up_copy.wait_recv()
        if step > 0:
            pl.when(low_ok)(up_copy.wait_recv)
        pl.when(low_ok & at.has_up)(up_copy.start)
        if step > 0:
            pl.when(high_ok)(down_copy.wait_recv)
        pl.when(high_ok & at.has_down)(down_copy.start)

    for flow in flows:
        if flow[0] == 0 and flow[2] == 0:
            run(flow)
    for w in range(3):
        own.append(
            pltpu.make_async_copy(w_refs[w].at[:, kept], w_outs[w].at[at.fs], own_sem.at[w])
        )
        own[-1].start()
    for offset in range(1, at.group):
        who = at.member_id((at.member + offset) % at.group)
        for part, (src, dst) in enumerate(((late_ref, late_out), (early_ref, early_out))):
            copy = remote(
                src, dst.at[at.member], tok_send.at[part, offset], tok_recv.at[part, offset], who
            )
            copy.start()
            tokens.append(copy)
    late_out[at.member] = late_ref[...]
    early_out[at.member] = early_ref[...]
    for flow in flows:
        if not (flow[0] == 0 and flow[2] == 0):
            run(flow)
    for copy in own + tokens:
        copy.wait()
    for copy in across:
        copy.wait_send()
    for flow in flows:
        up_copy, down_copy = flow_copies(flow)
        pl.when(flow[3] & at.has_up)(up_copy.wait_send)
        pl.when(flow[4] & at.has_down)(down_copy.wait_send)


def mixed_kernel(
    n_fs,
    n_tp,
    part_ref,
    grad_ref,
    gain_ref,
    out_ref,
    pair_in,
    pair_sum,
    sums_in,
    total,
    cot,
    pair_send,
    pair_recv,
    sum_send,
    sum_recv,
    cot_send,
    cot_recv,
    relay_send,
    relay_recv,
):
    at = Place(n_fs, n_tp)
    chips = at.group // PAIR
    partner = at.member_id(at.member + 1 - 2 * at.core)
    at.enter(False)

    def chip_at(offset):
        return (at.chip + offset) % chips

    def member_at(offset):
        return chip_at(offset) * PAIR + at.core

    order = list(range(1, chips)) + [0]
    halves = {}
    for offset in order:
        theirs = chip_at(offset) * PAIR + 1 - at.core
        halves[offset] = remote(
            part_ref.at[theirs],
            pair_in.at[offset],
            pair_send.at[offset],
            pair_recv.at[offset],
            partner,
        )
        halves[offset].start()
    sums = []
    for offset in order:
        halves[offset].wait_recv()
        both = part_ref[member_at(offset)].astype(jnp.float32) + pair_in[offset].astype(jnp.float32)
        if offset == 0:
            total[...] = both
            continue
        pair_sum[offset] = both.astype(jnp.bfloat16)
        copy = remote(
            pair_sum.at[offset],
            sums_in.at[offset],
            sum_send.at[offset],
            sum_recv.at[offset],
            at.member_id(member_at(offset)),
        )
        copy.start()
        sums.append(copy)
    for offset, copy in zip(order, sums):
        copy.wait_recv()
        total[...] += sums_in[offset].astype(jnp.float32)
    mixed = total[...].astype(jnp.bfloat16).astype(jnp.float32)
    inverse = inverse_rms(mixed)
    weighted = 0.5 * grad_ref[...].astype(jnp.float32) * gain_ref[...]
    cot[...] = (
        inverse * weighted
        - mixed * inverse**3 * jnp.mean(weighted * mixed, axis=-1, keepdims=True)
    ).astype(jnp.bfloat16)
    sends = []
    for offset in order:
        who = partner if offset == 0 else at.member_id(member_at(offset))
        sends.append(
            remote(cot, out_ref.at[at.member], cot_send.at[offset], cot_recv.at[offset], who)
        )
        sends[-1].start()
    out_ref[at.member] = cot[...]
    relays = []
    for offset, copy in zip(order, sends):
        copy.wait_recv()
        if offset == 0:
            continue
        slot = member_at(chips - offset)
        relay = remote(
            out_ref.at[slot], out_ref.at[slot], relay_send.at[offset], relay_recv.at[offset], partner
        )
        relay.start()
        relays.append(relay)
    for relay in relays:
        relay.wait()
    for copy in list(halves.values()) + sums + sends:
        copy.wait_send()


def scatter_kernel(n_fs, n_tp, *refs):
    parts, tok_parts, outs, tok_outs = refs[:3], refs[3:5], refs[5:8], refs[8:10]
    below, above, given, total, tok_in = refs[10:15]
    tok_send, tok_recv, up_send, up_recv, down_send, down_recv, across_send, across_recv = refs[15:]
    at = Place(n_fs, n_tp)
    rows = parts[0].shape[1]
    piece = min(rows, 64)
    at.enter(True)

    def over_rows(body):
        @pl.loop(0, rows // piece)
        def _(i):
            body(pl.ds(pl.multiple_of(i * piece, piece), piece))

    def pass_on(w, slot, held, send, recv, is_first, who):
        def copy_from(src):
            return remote(src, held.at[w, slot], send.at[w, slot], recv.at[w, slot], who)

        @pl.when(is_first)
        def _():
            copy_from(parts[w].at[slot]).start()

        @pl.when(jnp.logical_not(is_first))
        def _():
            copy = copy_from(held.at[w, slot])
            copy.wait_recv()

            def add(span):
                held[w, slot, span] = (
                    held[w, slot, span].astype(jnp.float32)
                    + parts[w][slot, span].astype(jnp.float32)
                ).astype(jnp.bfloat16)

            over_rows(add)
            copy.start()

    def send_tokens(which):
        for offset in range(1, at.group):
            member = (at.member + offset) % at.group
            copy = remote(
                tok_parts[which].at[member],
                tok_in.at[which, offset],
                tok_send.at[which, offset],
                tok_recv.at[which, offset],
                at.member_id(member),
            )
            copy.start()
            tokens[which].append(copy)

    tokens = [[], []]
    for step in range(at.line_len - 1):
        top, bottom = at.line_len - 1 - step, step
        for w in range(3):
            for turn in range(PAIR):
                pl.when(at.line < top)(
                    functools.partial(
                        pass_on, w, top * PAIR + turn, below, up_send, up_recv,
                        at.line == 0, at.up,
                    )
                )
                pl.when(at.line > bottom)(
                    functools.partial(
                        pass_on, w, bottom * PAIR + turn, above, down_send, down_recv,
                        at.line == at.line_len - 1, at.down,
                    )
                )
                if step == 0 and w == 0 and turn == 0:
                    send_tokens(0)
                    send_tokens(1)
    for which in range(2):
        running = tok_parts[which][at.member].astype(jnp.float32)
        for offset, copy in enumerate(tokens[which], 1):
            copy.wait_recv()
            running = running + tok_in[which, offset].astype(jnp.float32)
        tok_outs[which][...] = running.astype(jnp.bfloat16)
    across = []
    for w in range(3):
        for side in (1 - at.side, at.side):
            slot = at.line * PAIR + side

            def first(span):
                total[span] = parts[w][slot, span].astype(jnp.float32)

            def arrive(held, send, recv, who):
                remote(
                    held.at[w, slot], held.at[w, slot], send.at[w, slot], recv.at[w, slot], who
                ).wait_recv()

                def add(span):
                    total[span] += held[w, slot, span].astype(jnp.float32)

                over_rows(add)

            over_rows(first)
            pl.when(at.has_down)(lambda: arrive(below, up_send, up_recv, at.up))
            pl.when(at.has_up)(lambda: arrive(above, down_send, down_recv, at.down))
            if len(across) == w:

                def give(span):
                    given[w, span] = total[span].astype(jnp.bfloat16)

                over_rows(give)
                copy = remote(
                    given.at[w], outs[w].at[at.side], across_send.at[w], across_recv.at[w], at.across
                )
                copy.start()
                across.append(copy)
            else:

                def keep(span):
                    outs[w][at.side, span] = total[span].astype(jnp.bfloat16)

                over_rows(keep)
    for copy in across:
        copy.wait()
    for copy in tokens[0] + tokens[1]:
        copy.wait_send()
    for step in range(at.line_len - 1):
        top, bottom = at.line_len - 1 - step, step
        for w in range(3):
            for turn in range(PAIR):
                up_slot, down_slot = top * PAIR + turn, bottom * PAIR + turn
                up_copy = remote(
                    below.at[w, up_slot], below.at[w, up_slot],
                    up_send.at[w, up_slot], up_recv.at[w, up_slot], at.up,
                )
                down_copy = remote(
                    above.at[w, down_slot], above.at[w, down_slot],
                    down_send.at[w, down_slot], down_recv.at[w, down_slot], at.down,
                )
                pl.when(at.line < top)(up_copy.wait_send)
                pl.when(at.line > bottom)(down_copy.wait_send)


def call(kernel, collective_id, operands, out_shapes, scratch, flops):
    in_vmem = pl.BlockSpec(memory_space=pltpu.VMEM)
    return pl.pallas_call(
        kernel,
        out_shape=out_shapes,
        in_specs=[in_vmem] * len(operands),
        out_specs=[in_vmem] * len(out_shapes),
        scratch_shapes=scratch,
        cost_estimate=pl.CostEstimate(flops=flops, bytes_accessed=0, transcendentals=0),
        compiler_params=pltpu.CompilerParams(
            collective_id=collective_id, has_side_effects=True, vmem_limit_bytes=VMEM_LIMIT
        ),
    )(*operands)


def per_device(
    n_fs,
    n_tp,
    late_input,
    early_input,
    early_grad,
    pre_gain,
    post_gain,
    gate_weight,
    up_weight,
    down_weight,
    gate_sum,
    up_sum,
    down_gradient_sum,
):
    tok_rows, model_width = late_input.shape
    shard_rows, hidden_width = gate_weight.shape
    half = hidden_width // PAIR
    group = PAIR * n_tp
    chips = group // PAIR
    line_len = n_fs // PAIR
    group_rows = group * tok_rows
    grad_scale = 1.0 / math.sqrt(tok_rows * n_tp * n_fs)
    dma = pltpu.SemaphoreType.DMA
    bf16 = jnp.bfloat16

    def shaped(*shape):
        return jax.ShapeDtypeStruct(shape, bf16)

    def normed_of(rows):
        values = rows.astype(jnp.float32)
        inverse = inverse_rms(values)
        return values, inverse, (values * inverse * pre_gain).astype(bf16)

    late_values, _, late_normed = normed_of(late_input)
    early_values, early_in_inverse, early_own = normed_of(early_input)
    tok_block = shaped(group, tok_rows, model_width)
    w_block = shaped(n_fs, shard_rows, half)
    late_rows, early_rows, gate_all, up_all, down_all = call(
        functools.partial(gather_kernel, n_fs, n_tp),
        0,
        (late_normed, early_own, gate_weight, up_weight, down_weight),
        [tok_block, tok_block, w_block, w_block, w_block],
        [
            dma((2, group)),
            dma((2, group)),
            dma((3,)),
            dma((3,)),
            dma((3, line_len, PAIR)),
            dma((3, line_len, PAIR)),
            dma((3, n_fs)),
        ],
        10**9,
    )
    late_rows = late_rows.reshape(group_rows, model_width)
    early_rows = early_rows.reshape(group_rows, model_width)
    gate_all, up_all, down_all = (
        full.reshape(model_width, half) for full in (gate_all, up_all, down_all)
    )

    def hidden_of(rows):
        gate_pre = jnp.dot(rows, gate_all, preferred_element_type=jnp.float32)
        up_pre = jnp.dot(rows, up_all, preferred_element_type=jnp.float32)
        return gate_pre, up_pre, (jax.nn.silu(gate_pre) * up_pre).astype(bf16)

    def by_owner(product):
        return product.astype(bf16).reshape(group, tok_rows, model_width)

    early_gate, early_up, early_hidden = hidden_of(early_rows)
    early_part = by_owner(contract_last(early_hidden, down_all))
    chip_block = pltpu.VMEM((chips, tok_rows, model_width), bf16)
    (cot_rows,) = call(
        functools.partial(mixed_kernel, n_fs, n_tp),
        1,
        (early_part, early_grad, post_gain.reshape(1, model_width)),
        [tok_block],
        [
            chip_block,
            chip_block,
            chip_block,
            pltpu.VMEM((tok_rows, model_width), jnp.float32),
            pltpu.VMEM((tok_rows, model_width), bf16),
        ]
        + [dma((chips,))] * 8,
        10**8,
    )
    cot_rows = cot_rows.reshape(group_rows, model_width)
    _, _, late_hidden = hidden_of(late_rows)
    late_part = by_owner(contract_last(late_hidden, down_all))
    hidden_cot = jnp.dot(cot_rows, down_all, preferred_element_type=jnp.float32)
    sigmoid_gate = jax.nn.sigmoid(early_gate)
    gate_cot = (
        hidden_cot * early_up * sigmoid_gate * (1.0 + early_gate * (1.0 - sigmoid_gate))
    ).astype(bf16)
    up_cot = (hidden_cot * early_gate * sigmoid_gate).astype(bf16)
    normed_part = by_owner(contract_last(gate_cot, gate_all) + contract_last(up_cot, up_all))
    grad_parts = [
        (grad_scale * contract_first(first_op, second_op))
        .astype(bf16)
        .reshape(n_fs, shard_rows, half)
        for first_op, second_op in (
            (early_rows, gate_cot),
            (early_rows, up_cot),
            (cot_rows, early_hidden),
        )
    ]
    own_tokens = shaped(tok_rows, model_width)
    own_shard = shaped(PAIR, shard_rows, half)
    line_block = pltpu.VMEM((3, n_fs, shard_rows, half), bf16)
    *grads, normed_cot, late_mixed = call(
        functools.partial(scatter_kernel, n_fs, n_tp),
        2,
        (*grad_parts, normed_part, late_part),
        [own_shard, own_shard, own_shard, own_tokens, own_tokens],
        [
            line_block,
            line_block,
            pltpu.VMEM((3, shard_rows, half), bf16),
            pltpu.VMEM((shard_rows, half), jnp.float32),
            pltpu.VMEM((2, group, tok_rows, model_width), bf16),
            dma((2, group)),
            dma((2, group)),
        ]
        + [dma((3, n_fs))] * 4
        + [dma((3,))] * 2,
        10**9,
    )
    late_mixed = late_mixed.astype(jnp.float32)
    late_output = (
        late_values + 0.5 * late_mixed * inverse_rms(late_mixed) * post_gain
    ).astype(bf16)
    weighted_in = normed_cot.astype(jnp.float32) * pre_gain
    early_input_grad = (
        early_grad.astype(jnp.float32)
        + early_in_inverse * weighted_in
        - early_values
        * early_in_inverse**3
        * jnp.mean(weighted_in * early_values, axis=-1, keepdims=True)
    ).astype(bf16)
    totals = [
        running + jnp.concatenate([grad[0], grad[1]], axis=1).astype(jnp.float32)
        for running, grad in zip((gate_sum, up_sum, down_gradient_sum), grads)
    ]
    return (late_output, early_input_grad, *totals)


def solution(mesh):
    in_specs = (
        P(("fs", "tp"), None),
        P(("fs", "tp"), None),
        P(("fs", "tp"), None),
        P(),
        P(),
        P("fs", "tp"),
        P("fs", "tp"),
        P("fs", "tp"),
        P("fs", "tp"),
        P("fs", "tp"),
        P("fs", "tp"),
    )
    out_specs = (
        P(("fs", "tp"), None),
        P(("fs", "tp"), None),
        P("fs", "tp"),
        P("fs", "tp"),
        P("fs", "tp"),
    )
    return jax.shard_map(
        functools.partial(per_device, mesh.shape["fs"], mesh.shape["tp"]),
        mesh=mesh, in_specs=in_specs, out_specs=out_specs, check_vma=False
    )
```

```python
import functools
import math

import jax
import jax.numpy as jnp
from jax import lax
from jax.experimental import pallas as pl
from jax.experimental.pallas import tpu as pltpu
from jax.sharding import PartitionSpec as P

NORM_EPS = 1e-06
PAIR = 2
MESH = pl.DeviceIdType.MESH
VMEM_LIMIT = 60 * 1024 * 1024


def contract_last(first_op, second_op):
    return lax.dot_general(
        first_op, second_op, (((1,), (1,)), ((), ())), preferred_element_type=jnp.float32
    )


def contract_first(first_op, second_op):
    return lax.dot_general(
        first_op, second_op, (((0,), (0,)), ((), ())), preferred_element_type=jnp.float32
    )


def inverse_rms(values):
    return lax.rsqrt(jnp.mean(values * values, axis=-1, keepdims=True) + NORM_EPS)


class Place:
    def __init__(self, n_fs, n_tp):
        self.line_len, self.n_tp = n_fs // PAIR, n_tp
        self.group = PAIR * n_tp
        self.fs, self.tp = lax.axis_index("fs"), lax.axis_index("tp")
        self.line, self.side = self.fs // PAIR, self.fs % PAIR
        self.member = self.side * n_tp + self.tp
        self.core = self.tp % PAIR
        self.chip = self.member // PAIR
        self.up = {"fs": self.fs + PAIR, "tp": self.tp}
        self.down = {"fs": self.fs - PAIR, "tp": self.tp}
        self.across = {"fs": self.line * PAIR + 1 - self.side, "tp": self.tp}
        self.has_up, self.has_down = self.line < self.line_len - 1, self.line > 0

    def member_id(self, member):
        return {"fs": self.line * PAIR + member // self.n_tp, "tp": member % self.n_tp}

    def enter(self, on_line):
        barrier = pltpu.get_barrier_semaphore()

        def greet(who):
            pl.semaphore_signal(barrier, inc=1, device_id=who, device_id_type=MESH)

        for offset in range(1, self.group):
            greet(self.member_id((self.member + offset) % self.group))
        if on_line:
            pl.when(self.has_up)(lambda: greet(self.up))
            pl.when(self.has_down)(lambda: greet(self.down))
        peers = self.group - 1
        if on_line:
            peers += self.has_up.astype(jnp.int32) + self.has_down.astype(jnp.int32)
        pl.semaphore_wait(barrier, peers)


def remote(src, dst, send_sem, recv_sem, who):
    return pltpu.make_async_remote_copy(
        src_ref=src,
        dst_ref=dst,
        send_sem=send_sem,
        recv_sem=recv_sem,
        device_id=who,
        device_id_type=MESH,
    )


def gather_kernel(
    n_fs,
    n_tp,
    late_ref,
    early_ref,
    *refs,
):
    w_refs, (late_out, early_out), w_outs = refs[:3], refs[3:5], refs[5:8]
    tok_send, tok_recv, own_sem, across_send, up_send, down_send, w_recv = refs[8:]
    at = Place(n_fs, n_tp)
    half = w_outs[0].shape[2]
    kept = pl.ds(pl.multiple_of(at.side * half, half), half)
    given = pl.ds(pl.multiple_of((1 - at.side) * half, half), half)
    at.enter(True)

    def slot_of(line, turn):
        return line * PAIR + (at.side if turn == 0 else 1 - at.side)

    def carry(w, slot, src, send_sem, who):
        return remote(src, w_outs[w].at[slot], send_sem, w_recv.at[w, slot], who)

    across, own, tokens = [], [], []
    for w in range(3):
        across.append(
            carry(w, at.fs, w_refs[w].at[:, given], across_send.at[w], at.across)
        )
        across[-1].start()
    flows = []
    for step in range(at.line_len):
        for w in range(3):
            for turn in range(PAIR):
                from_low, from_high = at.line - step, at.line + step
                low = jnp.maximum(from_low, 0)
                high = jnp.minimum(from_high, at.line_len - 1)
                flows.append((step, w, turn, from_low >= 0, from_high < at.line_len, low, high))

    def flow_copies(flow):
        step, w, turn, _, _, low, high = flow
        own_block = step == 0 and turn == 0
        copies = []
        for line, sems, who in ((low, up_send, at.up), (high, down_send, at.down)):
            slot = slot_of(line, turn)
            src = w_refs[w].at[:, kept] if own_block else w_outs[w].at[slot]
            copies.append(carry(w, slot, src, sems.at[w, step, turn], who))
        return copies

    def run(flow):
        step, w, turn, low_ok, high_ok, _, _ = flow
        up_copy, down_copy = flow_copies(flow)
        if step == 0 and turn == 1:
            up_copy.wait_recv()
        if step > 0:
            pl.when(low_ok)(up_copy.wait_recv)
        pl.when(low_ok & at.has_up)(up_copy.start)
        if step > 0:
            pl.when(high_ok)(down_copy.wait_recv)
        pl.when(high_ok & at.has_down)(down_copy.start)

    for flow in flows:
        if flow[0] == 0 and flow[2] == 0:
            run(flow)
    for w in range(3):
        own.append(
            pltpu.make_async_copy(w_refs[w].at[:, kept], w_outs[w].at[at.fs], own_sem.at[w])
        )
        own[-1].start()
    late_out[at.member] = late_ref[...]
    early_out[at.member] = early_ref[...]
    for flow in flows:
        if flow[0] == 0 and flow[2] == 1:
            run(flow)
    for offset in range(1, at.group):
        who = at.member_id((at.member + offset) % at.group)
        for part, (src, dst) in enumerate(((late_ref, late_out), (early_ref, early_out))):
            copy = remote(
                src, dst.at[at.member], tok_send.at[part, offset], tok_recv.at[part, offset], who
            )
            copy.start()
            tokens.append(copy)
    for flow in flows:
        if flow[0] > 0:
            run(flow)
    for copy in own + tokens:
        copy.wait()
    for copy in across:
        copy.wait_send()
    for flow in flows:
        up_copy, down_copy = flow_copies(flow)
        pl.when(flow[3] & at.has_up)(up_copy.wait_send)
        pl.when(flow[4] & at.has_down)(down_copy.wait_send)


def mixed_kernel(
    n_fs,
    n_tp,
    part_ref,
    grad_ref,
    gain_ref,
    out_ref,
    pair_in,
    pair_sum,
    sums_in,
    total,
    cot,
    pair_send,
    pair_recv,
    sum_send,
    sum_recv,
    cot_send,
    cot_recv,
    relay_send,
    relay_recv,
):
    at = Place(n_fs, n_tp)
    chips = at.group // PAIR
    partner = at.member_id(at.member + 1 - 2 * at.core)
    at.enter(False)

    def chip_at(offset):
        return (at.chip + offset) % chips

    def member_at(offset):
        return chip_at(offset) * PAIR + at.core

    order = list(range(1, chips)) + [0]
    halves = {}
    for offset in order:
        theirs = chip_at(offset) * PAIR + 1 - at.core
        halves[offset] = remote(
            part_ref.at[theirs],
            pair_in.at[offset],
            pair_send.at[offset],
            pair_recv.at[offset],
            partner,
        )
        halves[offset].start()
    sums = []
    for offset in order:
        halves[offset].wait_recv()
        both = part_ref[member_at(offset)].astype(jnp.float32) + pair_in[offset].astype(jnp.float32)
        if offset == 0:
            total[...] = both
            continue
        pair_sum[offset] = both.astype(jnp.bfloat16)
        copy = remote(
            pair_sum.at[offset],
            sums_in.at[offset],
            sum_send.at[offset],
            sum_recv.at[offset],
            at.member_id(member_at(offset)),
        )
        copy.start()
        sums.append(copy)
    for offset, copy in zip(order, sums):
        copy.wait_recv()
        total[...] += sums_in[offset].astype(jnp.float32)
    mixed = total[...].astype(jnp.bfloat16).astype(jnp.float32)
    inverse = inverse_rms(mixed)
    weighted = 0.5 * grad_ref[...].astype(jnp.float32) * gain_ref[...]
    cot[...] = (
        inverse * weighted
        - mixed * inverse**3 * jnp.mean(weighted * mixed, axis=-1, keepdims=True)
    ).astype(jnp.bfloat16)
    sends = []
    for offset in order:
        who = partner if offset == 0 else at.member_id(member_at(offset))
        sends.append(
            remote(cot, out_ref.at[at.member], cot_send.at[offset], cot_recv.at[offset], who)
        )
        sends[-1].start()
    out_ref[at.member] = cot[...]
    relays = []
    for offset, copy in zip(order, sends):
        copy.wait_recv()
        if offset == 0:
            continue
        slot = member_at(chips - offset)
        relay = remote(
            out_ref.at[slot], out_ref.at[slot], relay_send.at[offset], relay_recv.at[offset], partner
        )
        relay.start()
        relays.append(relay)
    for relay in relays:
        relay.wait()
    for copy in list(halves.values()) + sums + sends:
        copy.wait_send()


def scatter_kernel(n_fs, n_tp, grad_scale, *refs):
    cot_ref, hidden_ref = refs[:2]
    outs, tok_outs = refs[9:12], refs[12:14]
    staged = refs[14:21]
    early_ref, down_ref, gate_ref, up_ref, gate_w, up_w, late_ref = staged
    parts, below, above, given, total, gate_cot, up_cot, tok_parts, tok_in = refs[21:30]
    (
        stage_sem,
        tok_send,
        tok_recv,
        up_send,
        up_recv,
        down_send,
        down_recv,
        across_send,
        across_recv,
    ) = refs[30:]
    at = Place(n_fs, n_tp)
    rows, tok_rows = parts.shape[2], tok_parts.shape[2]
    piece = min(rows, 64)
    owners = min(at.group, 4)
    tile = owners * tok_rows
    loads = [
        pltpu.make_async_copy(src, dst, stage_sem.at[i])
        for i, (src, dst) in enumerate(zip(refs[2:9], staged))
    ]
    for load in loads:
        load.start()
    at.enter(True)

    def over_rows(body):
        @pl.loop(0, rows // piece)
        def _(i):
            body(pl.ds(pl.multiple_of(i * piece, piece), piece))

    def over_tokens(body):
        @pl.loop(0, at.group // owners)
        def _(i):
            body(pl.ds(pl.multiple_of(i * tile, tile), tile), pl.ds(i * owners, owners))

    def grad_part(w, left_ref, right_ref):
        @pl.loop(0, n_fs)
        def _(slot):
            left = left_ref[:, pl.ds(pl.multiple_of(slot * rows, rows), rows)]
            parts[w, slot] = (grad_scale * contract_first(left, right_ref[...])).astype(
                jnp.bfloat16
            )

    def slots_of(w):
        for step in range(at.line_len - 1):
            for turn in range(PAIR):
                side = 1 - at.side if turn == 0 else at.side
                top, bottom = at.line_len - 1 - step, step
                yield top, top * PAIR + side, bottom, bottom * PAIR + side

    def hop(w, slot, src, upward):
        held, send, recv, who = (
            (below, up_send, up_recv, at.up) if upward else (above, down_send, down_recv, at.down)
        )
        src = held.at[w, slot] if src is None else src
        return remote(src, held.at[w, slot], send.at[w, slot], recv.at[w, slot], who)

    def first_sends(w):
        @pl.when(at.line == 0)
        def _():
            for _, slot, _, _ in slots_of(w):
                hop(w, slot, parts.at[w, slot], True).start()

        @pl.when(at.line == at.line_len - 1)
        def _():
            for _, _, _, slot in slots_of(w):
                hop(w, slot, parts.at[w, slot], False).start()

    def pass_on(w, slot, upward):
        copy = hop(w, slot, None, upward)
        held = below if upward else above
        copy.wait_recv()

        def add(span):
            held[w, slot, span] = (
                held[w, slot, span].astype(jnp.float32) + parts[w, slot, span].astype(jnp.float32)
            ).astype(jnp.bfloat16)

        over_rows(add)
        copy.start()

    def middle_sends(w):
        for top, up_slot, bottom, down_slot in slots_of(w):
            pl.when((at.line > 0) & (at.line < top))(
                functools.partial(pass_on, w, up_slot, True)
            )
            pl.when((at.line < at.line_len - 1) & (at.line > bottom))(
                functools.partial(pass_on, w, down_slot, False)
            )

    tokens = [[], []]

    def send_tokens(which):
        for offset in range(1, at.group):
            member = (at.member + offset) % at.group
            copy = remote(
                tok_parts.at[which, member],
                tok_in.at[which, offset],
                tok_send.at[which, offset],
                tok_recv.at[which, offset],
                at.member_id(member),
            )
            copy.start()
            tokens[which].append(copy)

    def by_owner(product):
        return product.astype(jnp.bfloat16).reshape(owners, tok_rows, product.shape[-1])

    def cots(span, _):
        hidden_cot = jnp.dot(cot_ref[span], down_ref[...], preferred_element_type=jnp.float32)
        gate, up = gate_ref[span], up_ref[span]
        sigmoid = jax.nn.sigmoid(gate)
        gate_cot[span] = (hidden_cot * up * sigmoid * (1.0 + gate * (1.0 - sigmoid))).astype(
            jnp.bfloat16
        )
        up_cot[span] = (hidden_cot * gate * sigmoid).astype(jnp.bfloat16)

    def normed_part(span, owned):
        tok_parts[0, owned] = by_owner(
            contract_last(gate_cot[span], gate_w[...]) + contract_last(up_cot[span], up_w[...])
        )

    def late_part(span, owned):
        late = late_ref[span]
        gate = jnp.dot(late, gate_w[...], preferred_element_type=jnp.float32)
        up = jnp.dot(late, up_w[...], preferred_element_type=jnp.float32)
        hidden = (gate * jax.nn.sigmoid(gate) * up).astype(jnp.bfloat16)
        tok_parts[1, owned] = by_owner(contract_last(hidden, down_ref[...]))

    across = []

    def finish(w):
        for turn in range(PAIR):
            side = 1 - at.side if turn == 0 else at.side
            slot = at.line * PAIR + side

            def first(span):
                total[span] = parts[w, slot, span].astype(jnp.float32)

            def arrive(upward):
                held = below if upward else above
                hop(w, slot, None, upward).wait_recv()

                def add(span):
                    total[span] += held[w, slot, span].astype(jnp.float32)

                over_rows(add)

            over_rows(first)
            pl.when(at.has_down)(functools.partial(arrive, True))
            pl.when(at.has_up)(functools.partial(arrive, False))
            if turn == 0:

                def give(span):
                    given[w, span] = total[span].astype(jnp.bfloat16)

                over_rows(give)
                copy = remote(
                    given.at[w], outs[w].at[at.side], across_send.at[w], across_recv.at[w], at.across
                )
                copy.start()
                across.append(copy)
            else:

                def keep(span):
                    outs[w][at.side, span] = total[span].astype(jnp.bfloat16)

                over_rows(keep)

    grad_part(2, cot_ref, hidden_ref)
    first_sends(2)
    for load in loads[:4]:
        load.wait()
    over_tokens(cots)
    grad_part(0, early_ref, gate_cot)
    first_sends(0)
    grad_part(1, early_ref, up_cot)
    first_sends(1)
    for load in loads[4:]:
        load.wait()
    over_tokens(normed_part)
    send_tokens(0)
    middle_sends(2)
    over_tokens(late_part)
    send_tokens(1)
    middle_sends(0)
    finish(2)
    for which in range(2):
        running = tok_parts[which, at.member].astype(jnp.float32)
        for offset, copy in enumerate(tokens[which], 1):
            copy.wait_recv()
            running = running + tok_in[which, offset].astype(jnp.float32)
        tok_outs[which][...] = running.astype(jnp.bfloat16)
        if which == 0:
            middle_sends(1)
            finish(0)
    finish(1)
    for copy in across:
        copy.wait()
    for copy in tokens[0] + tokens[1]:
        copy.wait_send()
    for w in range(3):
        for top, up_slot, bottom, down_slot in slots_of(w):
            pl.when(at.line < top)(hop(w, up_slot, None, True).wait_send)
            pl.when(at.line > bottom)(hop(w, down_slot, None, False).wait_send)


def call(kernel, collective_id, operands, out_shapes, scratch, flops, n_any=0):
    in_vmem = pl.BlockSpec(memory_space=pltpu.VMEM)
    in_any = pl.BlockSpec(memory_space=pl.ANY)
    return pl.pallas_call(
        kernel,
        out_shape=out_shapes,
        in_specs=[in_vmem] * (len(operands) - n_any) + [in_any] * n_any,
        out_specs=[in_vmem] * len(out_shapes),
        scratch_shapes=scratch,
        cost_estimate=pl.CostEstimate(flops=flops, bytes_accessed=0, transcendentals=0),
        compiler_params=pltpu.CompilerParams(
            collective_id=collective_id, has_side_effects=True, vmem_limit_bytes=VMEM_LIMIT
        ),
    )(*operands)


def per_device(
    n_fs,
    n_tp,
    late_input,
    early_input,
    early_grad,
    pre_gain,
    post_gain,
    gate_weight,
    up_weight,
    down_weight,
    gate_sum,
    up_sum,
    down_gradient_sum,
):
    tok_rows, model_width = late_input.shape
    shard_rows, hidden_width = gate_weight.shape
    half = hidden_width // PAIR
    group = PAIR * n_tp
    chips = group // PAIR
    line_len = n_fs // PAIR
    group_rows = group * tok_rows
    grad_scale = 1.0 / math.sqrt(tok_rows * n_tp * n_fs)
    dma = pltpu.SemaphoreType.DMA
    bf16 = jnp.bfloat16

    def shaped(*shape):
        return jax.ShapeDtypeStruct(shape, bf16)

    def normed_of(rows):
        values = rows.astype(jnp.float32)
        inverse = inverse_rms(values)
        return values, inverse, (values * inverse * pre_gain).astype(bf16)

    late_values, _, late_normed = normed_of(late_input)
    early_values, early_in_inverse, early_own = normed_of(early_input)
    tok_block = shaped(group, tok_rows, model_width)
    w_block = shaped(n_fs, shard_rows, half)
    late_rows, early_rows, gate_all, up_all, down_all = call(
        functools.partial(gather_kernel, n_fs, n_tp),
        0,
        (late_normed, early_own, gate_weight, up_weight, down_weight),
        [tok_block, tok_block, w_block, w_block, w_block],
        [
            dma((2, group)),
            dma((2, group)),
            dma((3,)),
            dma((3,)),
            dma((3, line_len, PAIR)),
            dma((3, line_len, PAIR)),
            dma((3, n_fs)),
        ],
        10**9,
    )
    late_rows = late_rows.reshape(group_rows, model_width)
    early_rows = early_rows.reshape(group_rows, model_width)
    gate_all, up_all, down_all = (
        full.reshape(model_width, half) for full in (gate_all, up_all, down_all)
    )

    def hidden_of(rows):
        gate_pre = jnp.dot(rows, gate_all, preferred_element_type=jnp.float32)
        up_pre = jnp.dot(rows, up_all, preferred_element_type=jnp.float32)
        return gate_pre, up_pre, (jax.nn.silu(gate_pre) * up_pre).astype(bf16)

    def by_owner(product):
        return product.astype(bf16).reshape(group, tok_rows, model_width)

    early_gate, early_up, early_hidden = hidden_of(early_rows)
    early_part = by_owner(contract_last(early_hidden, down_all))
    chip_block = pltpu.VMEM((chips, tok_rows, model_width), bf16)
    (cot_rows,) = call(
        functools.partial(mixed_kernel, n_fs, n_tp),
        1,
        (early_part, early_grad, post_gain.reshape(1, model_width)),
        [tok_block],
        [
            chip_block,
            chip_block,
            chip_block,
            pltpu.VMEM((tok_rows, model_width), jnp.float32),
            pltpu.VMEM((tok_rows, model_width), bf16),
        ]
        + [dma((chips,))] * 8,
        10**8,
    )
    cot_rows = cot_rows.reshape(group_rows, model_width)
    staged = (early_rows, down_all, early_gate, early_up, gate_all, up_all, late_rows)
    own_tokens = shaped(tok_rows, model_width)
    own_shard = shaped(PAIR, shard_rows, half)
    line_block = pltpu.VMEM((3, n_fs, shard_rows, half), bf16)
    *grads, normed_cot, late_mixed = call(
        functools.partial(scatter_kernel, n_fs, n_tp, grad_scale),
        2,
        (cot_rows, early_hidden, *staged),
        [own_shard, own_shard, own_shard, own_tokens, own_tokens],
        [pltpu.VMEM(array.shape, array.dtype) for array in staged]
        + [
            line_block,
            line_block,
            line_block,
            pltpu.VMEM((3, shard_rows, half), bf16),
            pltpu.VMEM((shard_rows, half), jnp.float32),
            pltpu.VMEM((group_rows, half), bf16),
            pltpu.VMEM((group_rows, half), bf16),
            pltpu.VMEM((2, group, tok_rows, model_width), bf16),
            pltpu.VMEM((2, group, tok_rows, model_width), bf16),
            dma((len(staged),)),
            dma((2, group)),
            dma((2, group)),
        ]
        + [dma((3, n_fs))] * 4
        + [dma((3,))] * 2,
        10**9,
        n_any=len(staged),
    )
    late_mixed = late_mixed.astype(jnp.float32)
    late_output = (
        late_values + 0.5 * late_mixed * inverse_rms(late_mixed) * post_gain
    ).astype(bf16)
    weighted_in = normed_cot.astype(jnp.float32) * pre_gain
    early_input_grad = (
        early_grad.astype(jnp.float32)
        + early_in_inverse * weighted_in
        - early_values
        * early_in_inverse**3
        * jnp.mean(weighted_in * early_values, axis=-1, keepdims=True)
    ).astype(bf16)
    totals = [
        running + jnp.concatenate([grad[0], grad[1]], axis=1).astype(jnp.float32)
        for running, grad in zip((gate_sum, up_sum, down_gradient_sum), grads)
    ]
    return (late_output, early_input_grad, *totals)


def solution(mesh):
    in_specs = (
        P(("fs", "tp"), None),
        P(("fs", "tp"), None),
        P(("fs", "tp"), None),
        P(),
        P(),
        P("fs", "tp"),
        P("fs", "tp"),
        P("fs", "tp"),
        P("fs", "tp"),
        P("fs", "tp"),
        P("fs", "tp"),
    )
    out_specs = (
        P(("fs", "tp"), None),
        P(("fs", "tp"), None),
        P("fs", "tp"),
        P("fs", "tp"),
        P("fs", "tp"),
    )
    return jax.shard_map(
        functools.partial(per_device, mesh.shape["fs"], mesh.shape["tp"]),
        mesh=mesh, in_specs=in_specs, out_specs=out_specs, check_vma=False
    )
```

```python
import functools
import math

import jax
import jax.numpy as jnp
from jax import lax
from jax.experimental import pallas as pl
from jax.experimental.pallas import tpu as pltpu
from jax.sharding import PartitionSpec as P

NORM_EPS = 1e-06
PAIR = 2
MESH = pl.DeviceIdType.MESH
VMEM_LIMIT = 60 * 1024 * 1024


def contract_last(first_op, second_op):
    return lax.dot_general(
        first_op, second_op, (((1,), (1,)), ((), ())), preferred_element_type=jnp.float32
    )


def contract_first(first_op, second_op):
    return lax.dot_general(
        first_op, second_op, (((0,), (0,)), ((), ())), preferred_element_type=jnp.float32
    )


def inverse_rms(values):
    return lax.rsqrt(jnp.mean(values * values, axis=-1, keepdims=True) + NORM_EPS)


class Place:
    def __init__(self, n_fs, n_tp):
        self.line_len, self.n_tp = n_fs // PAIR, n_tp
        self.group = PAIR * n_tp
        self.fs, self.tp = lax.axis_index("fs"), lax.axis_index("tp")
        self.line, self.side = self.fs // PAIR, self.fs % PAIR
        self.member = self.side * n_tp + self.tp
        self.core = self.tp % PAIR
        self.chip = self.member // PAIR
        self.up = {"fs": self.fs + PAIR, "tp": self.tp}
        self.down = {"fs": self.fs - PAIR, "tp": self.tp}
        self.across = {"fs": self.line * PAIR + 1 - self.side, "tp": self.tp}
        self.has_up, self.has_down = self.line < self.line_len - 1, self.line > 0

    def member_id(self, member):
        return {"fs": self.line * PAIR + member // self.n_tp, "tp": member % self.n_tp}

    def enter(self, on_line):
        barrier = pltpu.get_barrier_semaphore()

        def greet(who):
            pl.semaphore_signal(barrier, inc=1, device_id=who, device_id_type=MESH)

        for offset in range(1, self.group):
            greet(self.member_id((self.member + offset) % self.group))
        if on_line:
            pl.when(self.has_up)(lambda: greet(self.up))
            pl.when(self.has_down)(lambda: greet(self.down))
        peers = self.group - 1
        if on_line:
            peers += self.has_up.astype(jnp.int32) + self.has_down.astype(jnp.int32)
        pl.semaphore_wait(barrier, peers)


def remote(src, dst, send_sem, recv_sem, who):
    return pltpu.make_async_remote_copy(
        src_ref=src,
        dst_ref=dst,
        send_sem=send_sem,
        recv_sem=recv_sem,
        device_id=who,
        device_id_type=MESH,
    )


def gather_kernel(
    n_fs,
    n_tp,
    late_ref,
    early_ref,
    gain_ref,
    *refs,
):
    w_refs, (late_out, early_out), w_outs = refs[:3], refs[3:5], refs[5:8]
    gate_out, up_out, hidden_out, normed = refs[8:12]
    tok_send, tok_recv, own_sem, across_send, up_send, down_send, w_recv = refs[12:]
    at = Place(n_fs, n_tp)
    half = w_outs[0].shape[2]
    kept = pl.ds(pl.multiple_of(at.side * half, half), half)
    given = pl.ds(pl.multiple_of((1 - at.side) * half, half), half)
    at.enter(True)

    def slot_of(line, turn):
        return line * PAIR + (at.side if turn == 0 else 1 - at.side)

    def carry(w, slot, src, send_sem, who):
        return remote(src, w_outs[w].at[slot], send_sem, w_recv.at[w, slot], who)

    across, own, tokens = [], [], []
    for w in range(3):
        across.append(
            carry(w, at.fs, w_refs[w].at[:, given], across_send.at[w], at.across)
        )
        across[-1].start()
    flows = []
    for step in range(at.line_len):
        for w in range(3):
            for turn in range(PAIR):
                from_low, from_high = at.line - step, at.line + step
                low = jnp.maximum(from_low, 0)
                high = jnp.minimum(from_high, at.line_len - 1)
                flows.append((step, w, turn, from_low >= 0, from_high < at.line_len, low, high))

    def flow_copies(flow):
        step, w, turn, _, _, low, high = flow
        own_block = step == 0 and turn == 0
        copies = []
        for line, sems, who in ((low, up_send, at.up), (high, down_send, at.down)):
            slot = slot_of(line, turn)
            src = w_refs[w].at[:, kept] if own_block else w_outs[w].at[slot]
            copies.append(carry(w, slot, src, sems.at[w, step, turn], who))
        return copies

    def run(flow):
        step, w, turn, low_ok, high_ok, _, _ = flow
        up_copy, down_copy = flow_copies(flow)
        if step == 0 and turn == 1:
            up_copy.wait_recv()
        if step > 0:
            pl.when(low_ok)(up_copy.wait_recv)
        pl.when(low_ok & at.has_up)(up_copy.start)
        if step > 0:
            pl.when(high_ok)(down_copy.wait_recv)
        pl.when(high_ok & at.has_down)(down_copy.start)

    def run_where(weights, turns, forwarded):
        for flow in flows:
            if flow[1] in weights and flow[2] in turns and (flow[0] > 0) == forwarded:
                run(flow)

    run_where((0, 1), (0,), False)
    for w in range(3):
        own.append(
            pltpu.make_async_copy(w_refs[w].at[:, kept], w_outs[w].at[at.fs], own_sem.at[w])
        )
        own[-1].start()
    for part, (src, dst) in enumerate(((late_ref, late_out), (early_ref, early_out))):
        values = src[...].astype(jnp.float32)
        normed[part] = (values * inverse_rms(values) * gain_ref[...]).astype(jnp.bfloat16)
        dst[at.member] = normed[part]
    run_where((0, 1), (1,), False)
    for part, dst in ((1, early_out), (0, late_out)):
        for offset in range(1, at.group):
            copy = remote(
                normed.at[part],
                dst.at[at.member],
                tok_send.at[part, offset],
                tok_recv.at[part, offset],
                at.member_id((at.member + offset) % at.group),
            )
            copy.start()
            tokens.append(copy)
    run_where((0,), (0, 1), True)
    run_where((2,), (0, 1), False)
    run_where((1,), (0, 1), True)
    for copy in own:
        copy.wait()
    for copy in tokens[: at.group - 1]:
        copy.wait_recv()
    owners = min(at.group, 4)
    tile = owners * early_ref.shape[0]

    @pl.loop(0, at.group // owners)
    def _(i):
        span = pl.ds(pl.multiple_of(i * tile, tile), tile)
        rows = early_out[pl.ds(i * owners, owners)].reshape(tile, early_ref.shape[1])

        def product(w):
            return jnp.dot(
                rows, w_outs[w][...].reshape(-1, half), preferred_element_type=jnp.float32
            )

        gate, up = product(0), product(1)
        gate_out[span] = gate
        up_out[span] = up
        hidden_out[span] = (gate * jax.nn.sigmoid(gate) * up).astype(jnp.bfloat16)

    run_where((2,), (0, 1), True)
    for copy in tokens[at.group - 1 :]:
        copy.wait_recv()
    for copy in tokens:
        copy.wait_send()
    for copy in across:
        copy.wait_send()
    for flow in flows:
        up_copy, down_copy = flow_copies(flow)
        pl.when(flow[3] & at.has_up)(up_copy.wait_send)
        pl.when(flow[4] & at.has_down)(down_copy.wait_send)


def mixed_kernel(
    n_fs,
    n_tp,
    part_ref,
    grad_ref,
    gain_ref,
    out_ref,
    pair_in,
    pair_sum,
    sums_in,
    total,
    cot,
    pair_send,
    pair_recv,
    sum_send,
    sum_recv,
    cot_send,
    cot_recv,
    relay_send,
    relay_recv,
):
    at = Place(n_fs, n_tp)
    chips = at.group // PAIR
    partner = at.member_id(at.member + 1 - 2 * at.core)
    at.enter(False)

    def chip_at(offset):
        return (at.chip + offset) % chips

    def member_at(offset):
        return chip_at(offset) * PAIR + at.core

    order = list(range(1, chips)) + [0]
    halves = {}
    for offset in order:
        theirs = chip_at(offset) * PAIR + 1 - at.core
        halves[offset] = remote(
            part_ref.at[theirs],
            pair_in.at[offset],
            pair_send.at[offset],
            pair_recv.at[offset],
            partner,
        )
        halves[offset].start()
    sums = []
    for offset in order:
        halves[offset].wait_recv()
        both = part_ref[member_at(offset)].astype(jnp.float32) + pair_in[offset].astype(jnp.float32)
        if offset == 0:
            total[...] = both
            continue
        pair_sum[offset] = both.astype(jnp.bfloat16)
        copy = remote(
            pair_sum.at[offset],
            sums_in.at[offset],
            sum_send.at[offset],
            sum_recv.at[offset],
            at.member_id(member_at(offset)),
        )
        copy.start()
        sums.append(copy)
    for offset, copy in zip(order, sums):
        copy.wait_recv()
        total[...] += sums_in[offset].astype(jnp.float32)
    mixed = total[...].astype(jnp.bfloat16).astype(jnp.float32)
    inverse = inverse_rms(mixed)
    weighted = 0.5 * grad_ref[...].astype(jnp.float32) * gain_ref[...]
    cot[...] = (
        inverse * weighted
        - mixed * inverse**3 * jnp.mean(weighted * mixed, axis=-1, keepdims=True)
    ).astype(jnp.bfloat16)
    sends = []
    for offset in order:
        who = partner if offset == 0 else at.member_id(member_at(offset))
        sends.append(
            remote(cot, out_ref.at[at.member], cot_send.at[offset], cot_recv.at[offset], who)
        )
        sends[-1].start()
    out_ref[at.member] = cot[...]
    relays = []
    for offset, copy in zip(order, sends):
        copy.wait_recv()
        if offset == 0:
            continue
        slot = member_at(chips - offset)
        relay = remote(
            out_ref.at[slot], out_ref.at[slot], relay_send.at[offset], relay_recv.at[offset], partner
        )
        relay.start()
        relays.append(relay)
    for relay in relays:
        relay.wait()
    for copy in list(halves.values()) + sums + sends:
        copy.wait_send()


def scatter_kernel(n_fs, n_tp, grad_scale, *refs):
    cot_ref, hidden_ref = refs[:2]
    outs, tok_outs = refs[9:12], refs[12:14]
    staged = refs[14:21]
    early_ref, down_ref, gate_ref, up_ref, gate_w, up_w, late_ref = staged
    parts, below, above, given, total, gate_cot, up_cot, tok_parts, tok_in = refs[21:30]
    (
        stage_sem,
        tok_send,
        tok_recv,
        up_send,
        up_recv,
        down_send,
        down_recv,
        across_send,
        across_recv,
    ) = refs[30:]
    at = Place(n_fs, n_tp)
    rows, tok_rows = parts.shape[2], tok_parts.shape[2]
    piece = min(rows, 64)
    owners = min(at.group, 4)
    tile = owners * tok_rows
    loads = [
        pltpu.make_async_copy(src, dst, stage_sem.at[i])
        for i, (src, dst) in enumerate(zip(refs[2:9], staged))
    ]
    for load in loads:
        load.start()
    at.enter(True)

    def over_rows(body):
        @pl.loop(0, rows // piece)
        def _(i):
            body(pl.ds(pl.multiple_of(i * piece, piece), piece))

    def over_tokens(body):
        @pl.loop(0, at.group // owners)
        def _(i):
            body(pl.ds(pl.multiple_of(i * tile, tile), tile), pl.ds(i * owners, owners))

    def grad_part(w, left_ref, right_ref):
        @pl.loop(0, n_fs)
        def _(slot):
            left = left_ref[:, pl.ds(pl.multiple_of(slot * rows, rows), rows)]
            parts[w, slot] = (grad_scale * contract_first(left, right_ref[...])).astype(
                jnp.bfloat16
            )

    def slots_of(w):
        for step in range(at.line_len - 1):
            for turn in range(PAIR):
                side = 1 - at.side if turn == 0 else at.side
                top, bottom = at.line_len - 1 - step, step
                yield top, top * PAIR + side, bottom, bottom * PAIR + side

    def hop(w, slot, src, upward):
        held, send, recv, who = (
            (below, up_send, up_recv, at.up) if upward else (above, down_send, down_recv, at.down)
        )
        src = held.at[w, slot] if src is None else src
        return remote(src, held.at[w, slot], send.at[w, slot], recv.at[w, slot], who)

    def first_sends(w):
        @pl.when(at.line == 0)
        def _():
            for _, slot, _, _ in slots_of(w):
                hop(w, slot, parts.at[w, slot], True).start()

        @pl.when(at.line == at.line_len - 1)
        def _():
            for _, _, _, slot in slots_of(w):
                hop(w, slot, parts.at[w, slot], False).start()

    def pass_on(w, slot, upward):
        copy = hop(w, slot, None, upward)
        held = below if upward else above
        copy.wait_recv()

        def add(span):
            held[w, slot, span] = (
                held[w, slot, span].astype(jnp.float32) + parts[w, slot, span].astype(jnp.float32)
            ).astype(jnp.bfloat16)

        over_rows(add)
        copy.start()

    def middle_sends(w):
        for top, up_slot, bottom, down_slot in slots_of(w):
            pl.when((at.line > 0) & (at.line < top))(
                functools.partial(pass_on, w, up_slot, True)
            )
            pl.when((at.line < at.line_len - 1) & (at.line > bottom))(
                functools.partial(pass_on, w, down_slot, False)
            )

    tokens = [[], []]

    def send_tokens(which):
        for offset in range(1, at.group):
            member = (at.member + offset) % at.group
            copy = remote(
                tok_parts.at[which, member],
                tok_in.at[which, offset],
                tok_send.at[which, offset],
                tok_recv.at[which, offset],
                at.member_id(member),
            )
            copy.start()
            tokens[which].append(copy)

    def by_owner(product):
        return product.astype(jnp.bfloat16).reshape(owners, tok_rows, product.shape[-1])

    def cots(span, _):
        hidden_cot = jnp.dot(cot_ref[span], down_ref[...], preferred_element_type=jnp.float32)
        gate, up = gate_ref[span], up_ref[span]
        sigmoid = jax.nn.sigmoid(gate)
        gate_cot[span] = (hidden_cot * up * sigmoid * (1.0 + gate * (1.0 - sigmoid))).astype(
            jnp.bfloat16
        )
        up_cot[span] = (hidden_cot * gate * sigmoid).astype(jnp.bfloat16)

    def normed_part(span, owned):
        tok_parts[0, owned] = by_owner(
            contract_last(gate_cot[span], gate_w[...]) + contract_last(up_cot[span], up_w[...])
        )

    def late_part(span, owned):
        late = late_ref[span]
        gate = jnp.dot(late, gate_w[...], preferred_element_type=jnp.float32)
        up = jnp.dot(late, up_w[...], preferred_element_type=jnp.float32)
        hidden = (gate * jax.nn.sigmoid(gate) * up).astype(jnp.bfloat16)
        tok_parts[1, owned] = by_owner(contract_last(hidden, down_ref[...]))

    across = []

    def finish(w):
        for turn in range(PAIR):
            side = 1 - at.side if turn == 0 else at.side
            slot = at.line * PAIR + side

            def first(span):
                total[span] = parts[w, slot, span].astype(jnp.float32)

            def arrive(upward):
                held = below if upward else above
                hop(w, slot, None, upward).wait_recv()

                def add(span):
                    total[span] += held[w, slot, span].astype(jnp.float32)

                over_rows(add)

            over_rows(first)
            pl.when(at.has_down)(functools.partial(arrive, True))
            pl.when(at.has_up)(functools.partial(arrive, False))
            if turn == 0:

                def give(span):
                    given[w, span] = total[span].astype(jnp.bfloat16)

                over_rows(give)
                copy = remote(
                    given.at[w], outs[w].at[at.side], across_send.at[w], across_recv.at[w], at.across
                )
                copy.start()
                across.append(copy)
            else:

                def keep(span):
                    outs[w][at.side, span] = total[span].astype(jnp.bfloat16)

                over_rows(keep)

    grad_part(2, cot_ref, hidden_ref)
    first_sends(2)
    for load in loads[:4]:
        load.wait()
    over_tokens(cots)
    grad_part(0, early_ref, gate_cot)
    first_sends(0)
    grad_part(1, early_ref, up_cot)
    first_sends(1)
    for load in loads[4:]:
        load.wait()
    over_tokens(normed_part)
    send_tokens(0)
    middle_sends(2)
    over_tokens(late_part)
    send_tokens(1)
    middle_sends(0)
    finish(2)
    for which in range(2):
        running = tok_parts[which, at.member].astype(jnp.float32)
        for offset, copy in enumerate(tokens[which], 1):
            copy.wait_recv()
            running = running + tok_in[which, offset].astype(jnp.float32)
        tok_outs[which][...] = running.astype(jnp.bfloat16)
        if which == 0:
            middle_sends(1)
            finish(0)
    finish(1)
    for copy in across:
        copy.wait()
    for copy in tokens[0] + tokens[1]:
        copy.wait_send()
    for w in range(3):
        for top, up_slot, bottom, down_slot in slots_of(w):
            pl.when(at.line < top)(hop(w, up_slot, None, True).wait_send)
            pl.when(at.line > bottom)(hop(w, down_slot, None, False).wait_send)


def call(kernel, collective_id, operands, out_shapes, scratch, flops, n_any=0):
    in_vmem = pl.BlockSpec(memory_space=pltpu.VMEM)
    in_any = pl.BlockSpec(memory_space=pl.ANY)
    return pl.pallas_call(
        kernel,
        out_shape=out_shapes,
        in_specs=[in_vmem] * (len(operands) - n_any) + [in_any] * n_any,
        out_specs=[in_vmem] * len(out_shapes),
        scratch_shapes=scratch,
        cost_estimate=pl.CostEstimate(flops=flops, bytes_accessed=0, transcendentals=0),
        compiler_params=pltpu.CompilerParams(
            collective_id=collective_id, has_side_effects=True, vmem_limit_bytes=VMEM_LIMIT
        ),
    )(*operands)


def per_device(
    n_fs,
    n_tp,
    late_input,
    early_input,
    early_grad,
    pre_gain,
    post_gain,
    gate_weight,
    up_weight,
    down_weight,
    gate_sum,
    up_sum,
    down_gradient_sum,
):
    tok_rows, model_width = late_input.shape
    shard_rows, hidden_width = gate_weight.shape
    half = hidden_width // PAIR
    group = PAIR * n_tp
    chips = group // PAIR
    line_len = n_fs // PAIR
    group_rows = group * tok_rows
    grad_scale = 1.0 / math.sqrt(tok_rows * n_tp * n_fs)
    dma = pltpu.SemaphoreType.DMA
    bf16 = jnp.bfloat16

    def shaped(*shape):
        return jax.ShapeDtypeStruct(shape, bf16)

    late_values = late_input.astype(jnp.float32)
    early_values = early_input.astype(jnp.float32)
    early_in_inverse = inverse_rms(early_values)
    preact = jax.ShapeDtypeStruct((group_rows, half), jnp.float32)
    tok_block = shaped(group, tok_rows, model_width)
    w_block = shaped(n_fs, shard_rows, half)
    late_rows, early_rows, gate_all, up_all, down_all, early_gate, early_up, early_hidden = call(
        functools.partial(gather_kernel, n_fs, n_tp),
        0,
        (
            late_input,
            early_input,
            pre_gain.reshape(1, model_width),
            gate_weight,
            up_weight,
            down_weight,
        ),
        [tok_block] * 2 + [w_block] * 3 + [preact, preact, shaped(group_rows, half)],
        [
            pltpu.VMEM((2, tok_rows, model_width), bf16),
            dma((2, group)),
            dma((2, group)),
            dma((3,)),
            dma((3,)),
            dma((3, line_len, PAIR)),
            dma((3, line_len, PAIR)),
            dma((3, n_fs)),
        ],
        10**9,
    )
    late_rows = late_rows.reshape(group_rows, model_width)
    early_rows = early_rows.reshape(group_rows, model_width)
    gate_all, up_all, down_all = (
        full.reshape(model_width, half) for full in (gate_all, up_all, down_all)
    )

    def by_owner(product):
        return product.astype(bf16).reshape(group, tok_rows, model_width)

    early_part = by_owner(contract_last(early_hidden, down_all))
    chip_block = pltpu.VMEM((chips, tok_rows, model_width), bf16)
    (cot_rows,) = call(
        functools.partial(mixed_kernel, n_fs, n_tp),
        1,
        (early_part, early_grad, post_gain.reshape(1, model_width)),
        [tok_block],
        [
            chip_block,
            chip_block,
            chip_block,
            pltpu.VMEM((tok_rows, model_width), jnp.float32),
            pltpu.VMEM((tok_rows, model_width), bf16),
        ]
        + [dma((chips,))] * 8,
        10**8,
    )
    cot_rows = cot_rows.reshape(group_rows, model_width)
    staged = (early_rows, down_all, early_gate, early_up, gate_all, up_all, late_rows)
    own_tokens = shaped(tok_rows, model_width)
    own_shard = shaped(PAIR, shard_rows, half)
    line_block = pltpu.VMEM((3, n_fs, shard_rows, half), bf16)
    *grads, normed_cot, late_mixed = call(
        functools.partial(scatter_kernel, n_fs, n_tp, grad_scale),
        2,
        (cot_rows, early_hidden, *staged),
        [own_shard, own_shard, own_shard, own_tokens, own_tokens],
        [pltpu.VMEM(array.shape, array.dtype) for array in staged]
        + [
            line_block,
            line_block,
            line_block,
            pltpu.VMEM((3, shard_rows, half), bf16),
            pltpu.VMEM((shard_rows, half), jnp.float32),
            pltpu.VMEM((group_rows, half), bf16),
            pltpu.VMEM((group_rows, half), bf16),
            pltpu.VMEM((2, group, tok_rows, model_width), bf16),
            pltpu.VMEM((2, group, tok_rows, model_width), bf16),
            dma((len(staged),)),
            dma((2, group)),
            dma((2, group)),
        ]
        + [dma((3, n_fs))] * 4
        + [dma((3,))] * 2,
        10**9,
        n_any=len(staged),
    )
    late_mixed = late_mixed.astype(jnp.float32)
    late_output = (
        late_values + 0.5 * late_mixed * inverse_rms(late_mixed) * post_gain
    ).astype(bf16)
    weighted_in = normed_cot.astype(jnp.float32) * pre_gain
    early_input_grad = (
        early_grad.astype(jnp.float32)
        + early_in_inverse * weighted_in
        - early_values
        * early_in_inverse**3
        * jnp.mean(weighted_in * early_values, axis=-1, keepdims=True)
    ).astype(bf16)
    totals = [
        running + jnp.concatenate([grad[0], grad[1]], axis=1).astype(jnp.float32)
        for running, grad in zip((gate_sum, up_sum, down_gradient_sum), grads)
    ]
    return (late_output, early_input_grad, *totals)


def solution(mesh):
    in_specs = (
        P(("fs", "tp"), None),
        P(("fs", "tp"), None),
        P(("fs", "tp"), None),
        P(),
        P(),
        P("fs", "tp"),
        P("fs", "tp"),
        P("fs", "tp"),
        P("fs", "tp"),
        P("fs", "tp"),
        P("fs", "tp"),
    )
    out_specs = (
        P(("fs", "tp"), None),
        P(("fs", "tp"), None),
        P("fs", "tp"),
        P("fs", "tp"),
        P("fs", "tp"),
    )
    return jax.shard_map(
        functools.partial(per_device, mesh.shape["fs"], mesh.shape["tp"]),
        mesh=mesh, in_specs=in_specs, out_specs=out_specs, check_vma=False
    )
```
